32 devices in a mesh: rep: 2 (over x), fs: 8 (over z, y), tp: 2 (over core).
Axes of the slice: x: 2, y: 2, z: 4, core: 2. Of those that a mesh axis runs over, the one named last changes fastest.
Arguments:
- tokens: bfloat16 [4096, 2048], P(('rep', 'fs')), may hold values from -6 to 6
- first_gain: float32 [2048], replicated, may hold values from 0.1 to 1.9
- value_weight: float32 [2048, 1024], P('fs', 'tp'), may hold values from -0.125 to 0.125
- gate_weight: float32 [2048, 1024], P('fs', 'tp'), may hold values from -0.125 to 0.125
- value_scale: float32 [1024], P('tp'), may hold values from 0.5 to 2
- gate_scale: float32 [1024], P('tp'), may hold values from 0.5 to 2
- conv_taps: float32 [31, 1024], P(None, 'tp'), may hold values from -7 to 7
- chan_gain: float32 [1024], P('tp'), may hold values from 0.1 to 1.9
- mixout_weight: float32 [1024, 2048], P('tp', 'fs'), may hold values from -0.1875 to 0.1875
- mixout_scale: float32 [2048], P('fs'), may hold values from 0.5 to 2
- second_gain: float32 [2048], replicated, may hold values from 0.1 to 1.9
- up_weight: float32 [2048, 8192], P('fs', 'tp'), may hold values from -0.125 to 0.125
- up_scale: float32 [8192], P('tp'), may hold values from 0.5 to 2
- down_weight: float32 [8192, 2048], P('tp', 'fs'), may hold values from -0.0625 to 0.0625
- down_scale: float32 [2048], P('fs'), may hold values from 0.5 to 2
Outputs:
- layer_out: bfloat16 [4096, 2048], P(('rep', 'fs'))
The draws below stay inside these ranges and needn't reach their ends.
All inputs are finite; a program needn't handle non-finite values.
Results may differ from the reference program's by a relative error of at most 0.025.
Values may be sent and summed in bfloat16 or wider, within the bound.
No kernel may reach another device: no remote copies, remote signals or barrier semaphores. Data moves between devices by JAX's collectives and lax.ppermute only.
A program may use at most 128 MiB of HBM per device.

```python
import math
import jax
import jax.numpy as jnp
from jax import lax

D = 2048
CHANNELS = 1024
FF = 8192
CONV_K = 31
SEQ_LEN = 128
TOKENS = 4096
N_TP = 2


def draw_conv_taps(key, part):
    first, second = jax.random.split(jax.random.fold_in(key, 11))
    channel = jnp.arange(CHANNELS).astype(jnp.float32)
    rise = jnp.exp(jnp.log(6.0) * channel / max(CHANNELS - 1, 1))
    base = jnp.clip(jax.random.normal(first, (CONV_K, CHANNELS), jnp.float32), -4.0, 4.0)
    rough = jax.random.uniform(second, (CHANNELS,), jnp.float32, 0.5, 1.5)
    return (base * CONV_K ** (-0.5) * rise * rough).astype(jnp.float32)


def levels(key, dims, cuts, low, high):
    def one(dim, blocks):
        heights = jax.random.uniform(jax.random.fold_in(jax.random.fold_in(key, 6), dim), (blocks,), jnp.float32, low / len(cuts), high / len(cuts))
        return jnp.repeat(jnp.exp(heights), dims[dim] // blocks).reshape((-1,) + (1,) * (len(dims) - dim - 1))

    level = one(*cuts[0])
    for cut in cuts[1:]:
        level = level * one(*cut)
    return level


def scatter_about(own_key, extent, scale, reach, cuts=(), kind=jnp.bfloat16):
    factor_of = levels(own_key, extent, cuts, -0.22, 0.18) if cuts else 1.0
    values = jax.random.normal(own_key, extent, jnp.float32) * scale * factor_of
    return jnp.minimum(jnp.maximum(values, -reach), reach).astype(kind)


def setup_inputs(seed: int = 0) -> dict:
    keys = jax.random.split(jax.random.key(seed), 16)
    tokens = scatter_about(keys[0], (TOKENS, D), 1.0, 6.0, ((0, 16),))
    first_gain = jnp.clip(1.0 + 0.18 * jax.random.normal(keys[1], (D,), jnp.float32), 0.1, 1.9)
    value_weight = scatter_about(keys[2], (D, CHANNELS), D ** -0.5, 0.125, ((0, 8), (1, 2)), jnp.float32)
    gate_weight = scatter_about(keys[3], (D, CHANNELS), D ** -0.5, 0.125, ((0, 8), (1, 2)), jnp.float32)
    value_scale = jnp.clip(jnp.exp(math.log(2.0) - 1.3862944 * jax.random.uniform(keys[4], (CHANNELS,), jnp.float32) ** levels(keys[4], (CHANNELS,), ((0, 2),), -0.2, 0.2)), 0.5, 2.0)
    gate_scale = jnp.clip(jnp.exp(math.log(2.0) - 1.3862944 * jax.random.uniform(keys[5], (CHANNELS,), jnp.float32) ** levels(keys[5], (CHANNELS,), ((0, 2),), -0.2, 0.2)), 0.5, 2.0)
    conv_taps = draw_conv_taps(jax.random.fold_in(keys[15], 71), 0)
    chan_gain = jnp.clip(1.0 + 0.18 * jax.random.normal(keys[7], (CHANNELS,), jnp.float32), 0.1, 1.9)
    mixout_weight = scatter_about(keys[8], (CHANNELS, D), CHANNELS ** -0.5, 0.1875, ((0, 2), (1, 8)), jnp.float32)
    mixout_scale = jnp.clip(jnp.exp(math.log(2.0) - 1.3862944 * jax.random.uniform(keys[9], (D,), jnp.float32) ** levels(keys[9], (D,), ((0, 8),), -0.2, 0.2)), 0.5, 2.0)
    second_gain = jnp.clip(1.0 + 0.18 * jax.random.normal(keys[10], (D,), jnp.float32), 0.1, 1.9)
    up_weight = scatter_about(keys[11], (D, FF), D ** -0.5, 0.125, ((0, 8), (1, 2)), jnp.float32)
    up_scale = jnp.clip(jnp.exp(math.log(2.0) - 1.3862944 * jax.random.uniform(keys[12], (FF,), jnp.float32) ** levels(keys[12], (FF,), ((0, 2),), -0.2, 0.2)), 0.5, 2.0)
    down_weight = scatter_about(keys[13], (FF, D), FF ** -0.5, 0.0625, ((0, 2), (1, 8)), jnp.float32)
    down_scale = jnp.clip(jnp.exp(math.log(2.0) - 1.3862944 * jax.random.uniform(keys[14], (D,), jnp.float32) ** levels(keys[14], (D,), ((0, 8),), -0.2, 0.2)), 0.5, 2.0)
    return {"tokens": tokens, "first_gain": first_gain, "value_weight": value_weight, "gate_weight": gate_weight, "value_scale": value_scale, "gate_scale": gate_scale, "conv_taps": conv_taps, "chan_gain": chan_gain, "mixout_weight": mixout_weight, "mixout_scale": mixout_scale, "second_gain": second_gain, "up_weight": up_weight, "up_scale": up_scale, "down_weight": down_weight, "down_scale": down_scale}


def rms_rows(rows, gain):
    values = rows.astype(jnp.float32)
    scaled = values * lax.rsqrt(lax.optimization_barrier(jnp.mean(values * values, axis=-1, keepdims=True)) + 1e-05)
    return (scaled * gain).astype(jnp.bfloat16)

def rounded(scale):
    return lax.optimization_barrier(scale.astype(jnp.bfloat16)).astype(jnp.float32)

def causal_conv(signal, taps):
    width = signal.shape[1]
    seqs = signal.reshape(-1, SEQ_LEN, width)
    result = lax.conv_general_dilated(seqs, taps[:, None, :], (1,), [(taps.shape[0] - 1, 0)], dimension_numbers=('NWC', 'WIO', 'NWC'), feature_group_count=width, precision=lax.Precision.HIGHEST)
    return result.reshape(signal.shape)

def block_sum(left, right, scale):
    inner = left.shape[1] // N_TP
    total = jnp.zeros((left.shape[0], right.shape[1]), jnp.float32)
    for block in range(N_TP):
        term = jnp.dot(left[:, block * inner:(block + 1) * inner], right[block * inner:(block + 1) * inner], preferred_element_type=jnp.float32) * scale
        total = total + lax.optimization_barrier(term.astype(jnp.bfloat16)).astype(jnp.float32)
    return total

def reference(tokens, first_gain, value_weight, gate_weight, value_scale, gate_scale, conv_taps, chan_gain, mixout_weight, mixout_scale, second_gain, up_weight, up_scale, down_weight, down_scale):
    normed = rms_rows(tokens, first_gain)
    value_sum = jnp.dot(normed, value_weight.astype(jnp.bfloat16), preferred_element_type=jnp.float32)
    gate_sum = jnp.dot(normed, gate_weight.astype(jnp.bfloat16), preferred_element_type=jnp.float32)
    glu = value_sum * rounded(value_scale) * jax.nn.sigmoid(gate_sum * rounded(gate_scale))
    conv = causal_conv(glu, conv_taps)
    mean = lax.optimization_barrier(jnp.mean(conv, axis=1, keepdims=True))
    centred = conv - mean
    var = lax.optimization_barrier(jnp.mean(centred * centred, axis=1, keepdims=True))
    mixed_in = jax.nn.silu(centred * lax.rsqrt(var + 1e-05) * chan_gain).astype(jnp.bfloat16)
    mix_sum = block_sum(mixed_in, mixout_weight.astype(jnp.bfloat16), rounded(mixout_scale))
    middle = (tokens.astype(jnp.float32) + mix_sum).astype(jnp.bfloat16)
    normed2 = rms_rows(middle, second_gain)
    up_sum = jnp.dot(normed2, up_weight.astype(jnp.bfloat16), preferred_element_type=jnp.float32)
    hidden = jnp.square(jax.nn.relu(up_sum * rounded(up_scale))).astype(jnp.bfloat16)
    down_sum = block_sum(hidden, down_weight.astype(jnp.bfloat16), rounded(down_scale))
    return (middle.astype(jnp.float32) + down_sum).astype(jnp.bfloat16)
```

```python
import functools

import jax
import jax.numpy as jnp
from jax import lax
from jax.experimental import pallas as pl
from jax.experimental.pallas import tpu as pltpu
from jax.sharding import PartitionSpec as P

SEQ_LEN = 128
EPS = 1e-05
PAD = 16


ANY = pl.BlockSpec(memory_space=pl.ANY)
SMEM = pl.BlockSpec(memory_space=pltpu.SMEM)
VMEM = pl.BlockSpec(memory_space=pltpu.VMEM)
BF16 = jnp.bfloat16
F32 = jnp.float32


def rms_rows(rows, gain):
    values = rows.astype(F32)
    scaled = values * lax.rsqrt(jnp.mean(values * values, axis=-1, keepdims=True) + EPS)
    return (scaled * gain).astype(BF16)


def copy_all(pairs, sems):
    copies = [pltpu.make_async_copy(s, d, sems.at[i]) for i, (s, d) in enumerate(pairs)]
    for c in copies:
        c.start()
    for c in copies:
        c.wait()


def glu_conv_kernel(nb, rows, n_own, n_parts, idx, vs, gs, taps, *refs):
    own = refs[0]
    parts = refs[1 : 1 + n_parts]
    blocks = refs[1 + n_parts : 1 + n_parts + nb]
    conv_out, stat_out, x, w, padded, sems = refs[1 + n_parts + nb :]
    n = parts[0].shape[0]
    pairs = [(own, x.at[pl.ds(0, n_own)])]
    for p in range(n_parts):
        pairs.append((parts[p], x.at[pl.ds(pl.multiple_of(idx[nb + p], n), n)]))
    for b in range(nb):
        pairs.append((blocks[b], w.at[pl.ds(pl.multiple_of(idx[b] * rows, rows), rows)]))
    copy_all(pairs, sems)
    total, width = conv_out.shape
    n_seq = total // SEQ_LEN
    k = taps.shape[0]
    lead = padded.shape[1] - SEQ_LEN
    for s in range(n_seq):
        at = s * SEQ_LEN
        both = jnp.dot(x[at : at + SEQ_LEN, :], w[...], preferred_element_type=F32)
        glu = both[:, :width] * vs[...] * jax.nn.sigmoid(both[:, width:] * gs[...])
        padded[s, :lead, :] = jnp.zeros((lead, width), F32)
        padded[s, lead:, :] = glu
    for s in range(n_seq):
        at = s * SEQ_LEN
        acc = jnp.zeros((SEQ_LEN, width), F32)
        for j in range(k):
            start = lead - (k - 1) + j
            acc = acc + taps[j : j + 1, :] * padded[s, start : start + SEQ_LEN, :]
        conv_out[at : at + SEQ_LEN, :] = acc
    conv = conv_out[...]
    ones = jnp.ones((8, width), F32)
    dims = (((1,), (1,)), ((), ()))
    hi = lax.Precision.HIGHEST
    sums = lax.dot_general(ones, conv, dims, precision=hi, preferred_element_type=F32)
    squares = lax.dot_general(ones, conv * conv, dims, precision=hi, preferred_element_type=F32)
    row = lax.broadcasted_iota(jnp.int32, sums.shape, 0)
    stat_out[...] = jnp.where(row == 0, sums, squares)


def mix_kernel(nb, n_stats, reps, tps, n, channels, idx, gain, conv, *refs):
    stats = refs[:n_stats]
    blocks = refs[n_stats : n_stats + nb]
    outs = refs[n_stats + nb : n_stats + nb + tps]
    w, sems = refs[n_stats + nb + tps :]
    cols = blocks[0].shape[1]
    copy_all(
        [(blocks[b], w.at[:, pl.ds(pl.multiple_of(idx[b] * cols, cols), cols)]) for b in range(nb)],
        sems,
    )
    stat = stats[0][...]
    for s in stats[1:]:
        stat = stat + s[...]
    stat = stat.T
    mean = stat[:, 0:1] / channels
    var = stat[:, 1:2] / channels - mean * mean
    v = (conv[...] - mean) * lax.rsqrt(var + EPS) * gain[...]
    conv[...] = v / (1.0 + jnp.exp(-v))
    width = conv.shape[1]
    scale = w[width : width + 1, :].astype(F32)
    per = n * tps
    for k in range(tps):
        for r in range(reps):
            at = pl.multiple_of(r * per + idx[nb + k] * n, n)
            mixed = conv[pl.ds(at, n), :].astype(BF16)
            term = jnp.dot(mixed, w[:width, :], preferred_element_type=F32) * scale
            outs[k][r * n : (r + 1) * n, :] = term.astype(outs[k].dtype)


def ffn_kernel(nb, nd, n_tok, tps, idx, us, *refs):
    toks = refs[:n_tok]
    ups = refs[n_tok : n_tok + nb]
    downs = refs[n_tok + nb : n_tok + nb + nd]
    outs = refs[n_tok + nb + nd : n_tok + nb + nd + tps]
    x, wu, wd, sems = refs[n_tok + nb + nd + tps :]
    n = toks[0].shape[0]
    rows = ups[0].shape[0]
    cols = downs[0].shape[1]
    pairs = [(toks[t], x.at[pl.ds(t * n, n)]) for t in range(n_tok)]
    for b in range(nb):
        pairs.append((ups[b], wu.at[pl.ds(pl.multiple_of(idx[b] * rows, rows), rows)]))
    for b in range(nd):
        pairs.append((downs[b], wd.at[:, pl.ds(pl.multiple_of(idx[nb + b] * cols, cols), cols)]))
    copy_all(pairs, sems)
    units = wu.shape[1]
    scale = wd[units : units + 1, :].astype(F32)
    per = x.shape[0] // tps
    step = min(per, 256)
    for k in range(tps):
        for at in range(0, per, step):
            got = x[k * per + at : k * per + at + step, :]
            up = jnp.dot(got, wu[...], preferred_element_type=F32) * us[...]
            hidden = jnp.square(jnp.maximum(up, 0.0)).astype(BF16)
            term = jnp.dot(hidden, wd[:units, :], preferred_element_type=F32) * scale
            outs[k][at : at + step, :] = term.astype(outs[k].dtype)


def shift(array, axis, by):
    size = lax.axis_size(axis)
    return lax.ppermute(array, axis, [(i, (i + by) % size) for i in range(size)])


def on_device(
    tokens,
    first_gain,
    value_weight,
    gate_weight,
    value_scale,
    gate_scale,
    conv_taps,
    chan_gain,
    mixout_weight,
    mixout_scale,
    second_gain,
    up_weight,
    up_scale,
    down_weight,
    down_scale,
):
    reps, fss, tps = lax.axis_size("rep"), lax.axis_size("fs"), lax.axis_size("tp")
    outer = 4 if fss % 4 == 0 else fss
    inner = fss // outer
    pair = 2 if outer % 2 == 0 else 1
    xi, fi, ci = lax.axis_index("rep"), lax.axis_index("fs"), lax.axis_index("tp")
    zi, yi = fi // inner, fi % inner
    count, width = tokens.shape
    n = count // tps

    def z_shift(a, s):
        to = [(o * inner + i, ((o + s) % outer) * inner + i) for o in range(outer) for i in range(inner)]
        return lax.ppermute(a, "fs", to)

    def y_shift(a, s):
        to = [(o * inner + i, o * inner + (i + s) % inner) for o in range(outer) for i in range(inner)]
        return lax.ppermute(a, "fs", to)

    def pair_shift(a, s):
        to = [
            (o * inner + i, (o // pair * pair + (o + s) % pair) * inner + i)
            for o in range(outer)
            for i in range(inner)
        ]
        return lax.ppermute(a, "fs", to)

    sources = [(s, k) for s in range(outer) for k in range(inner)]
    places = [(zi - s) % outer * inner + (yi - k) % inner for s, k in sources]

    def gather(block_for):
        got = {(s, 0): z_shift(block_for(s), s) if s else block_for(0) for s in range(outer)}
        if inner <= 2:
            for s in range(outer):
                for k in range(1, inner):
                    got[s, k] = y_shift(got[s, 0], k)
        else:
            stack = jnp.stack([got[s, 0] for s in range(outer)])
            for k in range(1, inner):
                moved = y_shift(stack, k)
                for s in range(outer):
                    got[s, k] = moved[s]
        return [got[key] for key in sources]

    def take(a, at, size, axis):
        return lax.dynamic_slice_in_dim(a, at * size, size, axis=axis)

    mine = value_weight.shape[1] // reps
    vg = jnp.concatenate(
        [take(value_weight, xi, mine, 1).astype(BF16), take(gate_weight, xi, mine, 1).astype(BF16)], axis=1
    )
    vg_blocks = gather(lambda s: vg)

    def with_scale(block, scale):
        rows = jnp.broadcast_to(scale.astype(BF16)[None, :], (PAD, scale.shape[0]))
        return jnp.concatenate([block.astype(BF16), rows], axis=0)

    def columns(blocks):
        cols = blocks[0].shape[1]
        if cols % 128 == 0:
            return blocks, places
        joined = jnp.zeros((blocks[0].shape[0], cols * fss), BF16)
        for block, place in zip(blocks, places):
            joined = lax.dynamic_update_slice_in_dim(joined, block, place * cols, axis=1)
        return [joined], [jnp.zeros_like(places[0])]

    mix_own = with_scale(take(mixout_weight, xi, mine, 0), mixout_scale)
    mix_blocks, mix_places = columns(gather(lambda s: mix_own))

    normed = rms_rows(tokens, first_gain)
    half = take(normed, ci, n, 0)
    parts, offsets = [], []
    for r in range(1, reps):
        moved = shift(half, "rep", r)
        for k in range(tps):
            parts.append(shift(moved, "tp", k) if k else moved)
            offsets.append(r * count + (ci - k) % tps * n)

    groups = reps * pair
    units = up_weight.shape[1] // groups

    def up_for(s):
        return take(up_weight, xi * pair + (zi + s) % pair, units, 1).astype(BF16)

    def down_for(s):
        return with_scale(take(down_weight, xi * pair + (zi + s) % pair, units, 0), down_scale)

    up_blocks = gather(up_for)
    down_blocks, down_places = columns(gather(down_for))

    def rounded(scale, at, size):
        return take(scale, at, size, 0).astype(BF16).astype(F32)[None, :]

    total = reps * count
    rows = value_weight.shape[0]
    depth = rows * fss
    taps = take(conv_taps, xi, mine, 1)
    idx = jnp.stack(places + offsets).astype(jnp.int32)
    lead = -(-(conv_taps.shape[0] - 1) // 8) * 8
    conv, stat = pl.pallas_call(
        functools.partial(glu_conv_kernel, fss, rows, count, len(parts)),
        out_shape=(
            jax.ShapeDtypeStruct((total, mine), F32),
            jax.ShapeDtypeStruct((8, total), F32),
        ),
        in_specs=[SMEM, VMEM, VMEM, VMEM] + [ANY] * (1 + len(parts) + fss),
        out_specs=(VMEM, VMEM),
        scratch_shapes=[
            pltpu.VMEM((total, width), BF16),
            pltpu.VMEM((depth, 2 * mine), BF16),
            pltpu.VMEM((total // SEQ_LEN, SEQ_LEN + lead, mine), F32),
            pltpu.SemaphoreType.DMA((1 + len(parts) + fss,)),
        ],
        name="glu_conv",
    )(idx, rounded(value_scale, xi, mine), rounded(gate_scale, xi, mine), taps, normed, *parts, *vg_blocks)

    stats = [stat]
    for r in range(reps):
        for k in range(tps):
            if r or k:
                to = [
                    (i * tps + j, (i + r) % reps * tps + (j + k) % tps)
                    for i in range(reps)
                    for j in range(tps)
                ]
                stats.append((r, lax.ppermute(stat, ("rep", "tp"), to)))
    aligned = [stat]
    for r, s in stats[1:]:
        aligned.append(jnp.roll(s, r * count, axis=1) if r else s)

    n_mix = len(mix_blocks)
    idx = jnp.stack(mix_places + [(ci - k) % tps for k in range(tps)]).astype(jnp.int32)
    gain = take(chan_gain, xi, mine, 0)[None, :]
    mix_terms = pl.pallas_call(
        functools.partial(mix_kernel, n_mix, len(aligned), reps, tps, n, float(mine * reps * tps)),
        out_shape=tuple(
            jax.ShapeDtypeStruct((reps * n, width), BF16 if k else F32) for k in range(tps)
        ),
        in_specs=[SMEM, VMEM, VMEM] + [VMEM] * len(aligned) + [ANY] * n_mix,
        out_specs=tuple(VMEM for _ in range(tps)),
        scratch_shapes=[pltpu.VMEM((mine + PAD, width), BF16), pltpu.SemaphoreType.DMA((n_mix,))],
        name="mix",
    )(idx, gain, conv, *aligned, *mix_blocks)
    mix = mix_terms[0]
    for k in range(1, tps):
        mix = mix + shift(mix_terms[k], "tp", -k).astype(F32)
    mix_sum = mix[:n]
    for r in range(1, reps):
        mix_sum = mix_sum + shift(mix[r * n : (r + 1) * n].astype(BF16), "rep", -r).astype(F32)
    middle = (take(tokens, ci, n, 0).astype(F32) + mix_sum).astype(BF16)
    normed2 = rms_rows(middle, second_gain)

    per_q = [normed2] + [pair_shift(normed2, q) for q in range(1, pair)]
    local = []
    for q in range(pair):
        for r in range(reps):
            local.append(shift(per_q[q], "rep", r) if r else per_q[q])
    toks = []
    for k in range(tps):
        toks += [shift(t, "tp", k) if k else t for t in local]

    group = xi * pair + zi % pair
    n_down = len(down_blocks)
    idx = jnp.stack(places + down_places).astype(jnp.int32)
    per = len(local) * n
    terms = pl.pallas_call(
        functools.partial(ffn_kernel, fss, n_down, len(toks), tps),
        out_shape=tuple(jax.ShapeDtypeStruct((per, width), BF16 if k else F32) for k in range(tps)),
        in_specs=[SMEM, VMEM] + [ANY] * (len(toks) + fss + n_down),
        out_specs=tuple(VMEM for _ in range(tps)),
        scratch_shapes=[
            pltpu.VMEM((len(toks) * n, width), BF16),
            pltpu.VMEM((depth, units), BF16),
            pltpu.VMEM((units + PAD, width), BF16),
            pltpu.SemaphoreType.DMA((len(toks) + fss + n_down,)),
        ],
        name="ffn",
    )(idx, rounded(up_scale, group, units), *toks, *up_blocks, *down_blocks)
    acc = terms[0]
    for k in range(1, tps):
        acc = acc + shift(terms[k], "tp", -k).astype(F32)
    acc = acc.reshape(pair, reps, n, width)
    over_q = acc[:, 0]
    for r in range(1, reps):
        over_q = over_q + shift(acc[:, r].astype(BF16), "rep", -r).astype(F32)
    down_sum = over_q[0]
    for q in range(1, pair):
        down_sum = down_sum + pair_shift(over_q[q].astype(BF16), -q).astype(F32)
    own = (middle.astype(F32) + down_sum).astype(BF16)
    result = jnp.zeros((count, width), BF16)
    for k in range(tps):
        piece = shift(own, "tp", k) if k else own
        result = lax.dynamic_update_slice_in_dim(result, piece, (ci - k) % tps * n, axis=0)
    return result


def solution(mesh):
    placed = (
        P(("rep", "fs"), None),
        P(),
        P("fs", "tp"),
        P("fs", "tp"),
        P("tp"),
        P("tp"),
        P(None, "tp"),
        P("tp"),
        P("tp", "fs"),
        P("fs"),
        P(),
        P("fs", "tp"),
        P("tp"),
        P("tp", "fs"),
        P("fs"),
    )
    return jax.shard_map(
        on_device, mesh=mesh, in_specs=placed, out_specs=P(("rep", "fs"), None), check_vma=False
    )
```

```python
import functools

import jax
import jax.numpy as jnp
from jax import lax
from jax.experimental import pallas as pl
from jax.experimental.pallas import tpu as pltpu
from jax.sharding import PartitionSpec as P


SEQ_LEN = 128
EPS = 1e-05
PAD = 16


ANY = pl.BlockSpec(memory_space=pl.ANY)
SMEM = pl.BlockSpec(memory_space=pltpu.SMEM)
VMEM = pl.BlockSpec(memory_space=pltpu.VMEM)
BF16 = jnp.bfloat16
F32 = jnp.float32


def rms_rows(rows, gain):
    values = rows.astype(F32)
    scaled = values * lax.rsqrt(jnp.mean(values * values, axis=-1, keepdims=True) + EPS)
    return (scaled * gain).astype(BF16)


def start_all(pairs, sems):
    copies = [pltpu.make_async_copy(s, d, sems.at[i]) for i, (s, d) in enumerate(pairs)]
    for c in copies:
        c.start()
    return copies


def lanes(ref, index, width):
    if ref.shape[1] == width:
        return slice(None)
    return pl.ds(pl.multiple_of(index * width, width), width)


def wait_all(copies):
    for c in copies:
        c.wait()


def glu_conv_kernel(places, offsets, rows, n_own, pos, vs, gs, taps, *refs):
    nb, n_parts = len(places), len(offsets)
    own = refs[0]
    parts = refs[1 : 1 + n_parts]
    blocks = refs[1 + n_parts : 1 + n_parts + nb]
    conv_out, stat_out, x, w, padded, sems = refs[1 + n_parts + nb :]
    n = parts[0].shape[0]
    pairs = [(own, x.at[pl.ds(0, n_own)])]
    for p in range(n_parts):
        pairs.append((parts[p], x.at[pl.ds(pl.multiple_of(offsets[p](pos), n), n)]))
    for b in range(nb):
        pairs.append((blocks[b], w.at[pl.ds(pl.multiple_of(places[b](pos) * rows, rows), rows)]))
    wait_all(start_all(pairs, sems))
    total, width = conv_out.shape
    chan = lanes(vs, pos[0], width)
    vs_own = vs[:, chan].astype(BF16).astype(F32)
    gs_own = gs[:, chan].astype(BF16).astype(F32)
    n_seq = total // SEQ_LEN
    k = taps.shape[0]
    lead = padded.shape[1] - SEQ_LEN
    both = jnp.dot(x[...], w[...], preferred_element_type=F32)
    glu = both[:, :width] * vs_own * jax.nn.sigmoid(both[:, width:] * gs_own)
    for s in range(n_seq):
        padded[s, :lead, :] = jnp.zeros((lead, width), F32)
        padded[s, lead:, :] = glu[s * SEQ_LEN : (s + 1) * SEQ_LEN, :]
    for s in range(n_seq):
        at = s * SEQ_LEN
        acc = jnp.zeros((SEQ_LEN, width), F32)
        for j in range(k):
            start = lead - (k - 1) + j
            acc = acc + taps[j : j + 1, chan] * padded[s, start : start + SEQ_LEN, :]
        conv_out[at : at + SEQ_LEN, :] = acc
    conv = conv_out[...]
    sums = jnp.sum(conv, axis=1, keepdims=True)
    squares = jnp.sum(conv * conv, axis=1, keepdims=True)
    lane = lax.broadcasted_iota(jnp.int32, (total, 128), 1)
    stat_out[...] = jnp.where(lane == 0, sums, squares).T[:8, :]


def mix_kernel(places, turns, reps, tps, n, channels, pos, gain, conv, *refs):
    nb, n_stats = len(places), len(turns)
    stats = refs[:n_stats]
    blocks = refs[n_stats : n_stats + nb]
    outs = refs[n_stats + nb : n_stats + nb + tps]
    w, columns, sems = refs[n_stats + nb + tps :]
    cols = blocks[0].shape[1]
    copies = start_all(
        [(blocks[b], w.at[:, pl.ds(pl.multiple_of(places[b](pos) * cols, cols), cols)]) for b in range(nb)],
        sems,
    )
    width = conv.shape[1]
    stat = stats[0][...]
    per = n * tps
    for s, turn in zip(stats[1:], turns[1:]):
        blocks_of = [(q - turn) % reps for q in range(reps)]
        stat = stat + jnp.concatenate([s[:, q * per : (q + 1) * per] for q in blocks_of], axis=1)
    columns[...] = stat.T
    own_gain = gain[:, lanes(gain, pos[0], width)]
    wait_all(copies)
    scale = w[width : width + 1, :].astype(F32)
    mixed = []
    for k in range(tps):
        for r in range(reps):
            at = pl.multiple_of(r * per + lax.rem(pos[3] + tps - k, tps) * n, n)
            column = columns[pl.ds(at, n), :]
            mean = column[:, 0:1] / channels
            var = column[:, 1:2] / channels - mean * mean
            v = (conv[pl.ds(at, n), :] - mean) * lax.rsqrt(var + EPS) * own_gain
            mixed.append((v / (1.0 + jnp.exp(-v))).astype(BF16))
    mixed = jnp.concatenate(mixed, axis=0)
    term = (jnp.dot(mixed, w[:width, :], preferred_element_type=F32) * scale).astype(BF16)
    for k in range(tps):
        outs[k][...] = term[k * reps * n : (k + 1) * reps * n, :]


def up_kernel(places, n_tok, tps, pos, *refs):
    nb = len(places)
    scales = refs[:tps]
    refs = refs[tps:]
    toks = refs[:n_tok]
    ups = refs[n_tok : n_tok + tps * nb]
    out, x, wu, stage, sems, out_sems = refs[n_tok + tps * nb :]
    units = wu.shape[1] // tps
    rows = ups[0].shape[0]
    n = toks[0].shape[0]
    pairs = [(t, x.at[pl.ds(i * n, n)]) for i, t in enumerate(toks)]
    for k in range(tps):
        for b in range(nb):
            at = pl.ds(pl.multiple_of(places[b](pos) * rows, rows), rows)
            pairs.append((ups[k * nb + b], wu.at[at, pl.ds(k * units, units)]))
    copies = start_all(pairs, sems)
    wait_all(copies[:n_tok])
    step = min(x.shape[0], 512)
    writes = []
    for k in range(tps):
        wait_all(copies[n_tok + k * nb : n_tok + (k + 1) * nb])
        for at in range(0, x.shape[0], step):
            w = wu[:, k * units : (k + 1) * units]
            up = jnp.dot(x[at : at + step, :], w, preferred_element_type=F32) * scales[k][...].astype(BF16).astype(F32)
            stage[at : at + step, k * units : (k + 1) * units] = jnp.square(jnp.maximum(up, 0.0)).astype(BF16)
        cut = pl.ds(k * units, units)
        writes.append(pltpu.make_async_copy(stage.at[:, cut], out.at[:, cut], out_sems.at[k]))
        writes[-1].start()
    wait_all(writes)


def down_kernel(places, tps, order, n, kept_rows, pos, hidden, *refs):
    nd = len(places)
    downs = refs[: tps * nd]
    kept, sent, h, wd, ws, sems = refs[tps * nd :]
    cols = downs[0].shape[1]
    units = h.shape[1] // tps
    pairs = [(hidden, h)]
    for b in range(nd):
        at = pl.ds(pl.multiple_of(places[b](pos) * cols, cols), cols)
        for k in range(tps):
            pairs.append((downs[k * nd + b].at[pl.ds(0, units)], wd.at[pl.ds(k * units, units), at]))
        pairs.append((downs[b].at[pl.ds(units, PAD)], ws.at[:, at]))
    wait_all(start_all(pairs, sems))
    scale = ws[0:1, :].astype(F32)
    term = jnp.dot(h[...], wd[...], preferred_element_type=F32) * scale
    for j, to in enumerate(order):
        rows = term[j * n : (j + 1) * n, :]
        if to * n < kept_rows:
            kept[to * n : (to + 1) * n, :] = rows
        else:
            sent[to * n - kept_rows : (to + 1) * n - kept_rows, :] = rows.astype(BF16)


def final_kernel(inner, pair, cols, tps, pos, *refs):
    out = refs[-1]
    n_parts = 1 + inner
    base = pos[1] - lax.rem(pos[1], pair)
    for c in range(tps):
        parts = refs[c * n_parts : (c + 1) * n_parts]
        n = parts[0].shape[0]
        rows = pl.ds(pl.multiple_of(lax.rem(pos[3] + tps - c, tps) * n, n), n)
        wide = parts[0].shape[1]
        out[rows, pl.ds(pl.multiple_of(base * inner * cols, cols), wide)] = parts[0][...]
        for k in range(inner):
            for z in range(pair):
                block = (pair - base + z) * inner + lax.rem(pos[2] + inner - k, inner)
                at = pl.multiple_of(block * cols, cols)
                out[rows, pl.ds(at, cols)] = parts[1 + k][:, z * cols : (z + 1) * cols]


def shift(array, axis, by):
    size = lax.axis_size(axis)
    return lax.ppermute(array, axis, [(i, (i + by) % size) for i in range(size)])


def on_device(
    tokens,
    first_gain,
    value_weight,
    gate_weight,
    value_scale,
    gate_scale,
    conv_taps,
    chan_gain,
    mixout_weight,
    mixout_scale,
    second_gain,
    up_weight,
    up_scale,
    down_weight,
    down_scale,
):
    reps, fss, tps = lax.axis_size("rep"), lax.axis_size("fs"), lax.axis_size("tp")
    outer, pair = 4, 2
    inner = fss // outer
    xi, fi, ci = lax.axis_index("rep"), lax.axis_index("fs"), lax.axis_index("tp")
    zi, yi = fi // inner, fi % inner
    count, width = tokens.shape
    n = count // tps

    def along(a, to):
        return lax.ppermute(a, "fs", [(o * inner + i, to(o, i)) for o in range(outer) for i in range(inner)])

    def z_swap(a, m):
        return along(a, lambda o, i: (o ^ m) * inner + i)

    def y_shift(a, s):
        return along(a, lambda o, i: o * inner + (i + s) % inner)

    def pair_shift(a, s):
        return along(a, lambda o, i: (o // pair * pair + (o + s) % pair) * inner + i)

    pos = jnp.stack([xi, zi, yi, ci]).astype(jnp.int32)

    def spread(got):
        if inner <= 2:
            return [list(got.values())] + [[y_shift(b, k) for b in got.values()] for k in range(1, inner)]
        stack = jnp.stack(list(got.values()))
        moved = [y_shift(stack, k) for k in range(1, inner)]
        return [list(got.values())] + [[m[s] for s in range(outer)] for m in moved]

    def gather(block):
        got = {"0": block, "a": z_swap(block, 1), "b": z_swap(block, 2)}
        got["c"] = z_swap(got["b"], 1)
        return spread(got)

    def exchange(blocks):
        got = {"0": blocks[0]}
        for m in range(1, outer):
            got[str(m)] = z_swap(blocks[m % pair], m)
        return spread(got)

    def place(m, k):
        return lambda p: (p[1] ^ m) * inner + lax.rem(p[2] + inner - k, inner)

    all_places = [place(m, k) for k in range(inner) for m in range(outer)]

    def flat(blocks):
        return [b for row in blocks for b in row]

    def take(a, at, size, axis):
        return lax.dynamic_slice_in_dim(a, at * size, size, axis=axis)

    mine = value_weight.shape[1] // reps
    vg = jnp.concatenate(
        [take(value_weight, xi, mine, 1).astype(BF16), take(gate_weight, xi, mine, 1).astype(BF16)], axis=1
    )

    def channels_of(a):
        return a if mine % 128 == 0 else take(a, xi, mine, 1)

    vg_blocks = flat(gather(vg))

    def with_scale(block, scale):
        rows = jnp.broadcast_to(scale.astype(BF16)[None, :], (PAD, scale.shape[0]))
        return jnp.concatenate([block.astype(BF16), rows], axis=0)

    def columns(blocks, at):
        cols = blocks[0].shape[1]
        if cols % 128 == 0:
            return blocks, at
        joined = jnp.zeros((blocks[0].shape[0], cols * len(blocks)), BF16)
        for block, spot in zip(blocks, at):
            joined = lax.dynamic_update_slice_in_dim(joined, block, spot(pos) * cols, axis=1)
        return [joined], [lambda p: 0]

    mix_own = with_scale(take(mixout_weight, xi, mine, 0), mixout_scale)
    mix_blocks, mix_places = columns(flat(gather(mix_own)), all_places)

    normed = rms_rows(tokens, first_gain)
    half = take(normed, ci, n, 0)
    parts, offsets = [], []
    for r in range(1, reps):
        moved = shift(half, "rep", r)
        for k in range(tps):
            parts.append(shift(moved, "tp", k) if k else moved)
            offsets.append(lambda p, r=r, k=k: r * count + lax.rem(p[3] + tps - k, tps) * n)

    groups = reps * pair
    units = up_weight.shape[1] // groups

    at_pair = [xi * pair + (zi + s) % pair for s in range(pair)]
    ups = [take(up_weight, g, units, 1).astype(BF16) for g in at_pair]
    downs = [with_scale(take(down_weight, g, units, 0), down_scale) for g in at_pair]

    def share(parts):
        if tps == 2:
            return [[blocks, [shift(b, "tp", 1) for b in blocks]] for blocks in parts]
        shared = []
        for blocks in parts:
            stack = jnp.stack(blocks)
            moved = [shift(stack, "tp", k) for k in range(1, tps)]
            shared.append([blocks] + [[m[s] for s in range(len(blocks))] for m in moved])
        return shared

    up_blocks = exchange(ups)
    up_blocks = share(up_blocks)
    up_blocks = [b for k in range(tps) for part in up_blocks for b in part[k]]
    down_blocks = exchange(downs)
    down_blocks = share(down_blocks)
    own_scale = take(up_scale, at_pair[0], units, 0)[None, :]
    up_scales = [own_scale] + [shift(own_scale, "tp", k) for k in range(1, tps)]

    total = reps * count
    rows = value_weight.shape[0]
    depth = rows * fss
    lead = -(-(conv_taps.shape[0] - 1) // 8) * 8
    conv, stat = pl.pallas_call(
        functools.partial(glu_conv_kernel, all_places, offsets, rows, count),
        out_shape=(
            jax.ShapeDtypeStruct((total, mine), F32),
            jax.ShapeDtypeStruct((8, total), F32),
        ),
        in_specs=[SMEM, VMEM, VMEM, VMEM] + [ANY] * (1 + len(parts) + fss),
        out_specs=(VMEM, VMEM),
        scratch_shapes=[
            pltpu.VMEM((total, width), BF16),
            pltpu.VMEM((depth, 2 * mine), BF16),
            pltpu.VMEM((total // SEQ_LEN, SEQ_LEN + lead, mine), F32),
            pltpu.SemaphoreType.DMA((1 + len(parts) + fss,)),
        ],
        name="glu_conv",
    )(pos, channels_of(value_scale[None, :]), channels_of(gate_scale[None, :]), channels_of(conv_taps), normed, *parts, *vg_blocks)

    stats = [stat]
    for r in range(reps):
        for k in range(tps):
            if r or k:
                to = [
                    (i * tps + j, (i + r) % reps * tps + (j + k) % tps)
                    for i in range(reps)
                    for j in range(tps)
                ]
                stats.append((r, lax.ppermute(stat, ("rep", "tp"), to)))
    turns = [0] + [r for r, _ in stats[1:]]
    aligned = [stat] + [t for _, t in stats[1:]]
    n_mix = len(mix_blocks)
    mix_terms = pl.pallas_call(
        functools.partial(mix_kernel, mix_places, turns, reps, tps, n, float(mine * reps * tps)),
        out_shape=tuple(jax.ShapeDtypeStruct((reps * n, width), BF16) for _ in range(tps)),
        in_specs=[SMEM, VMEM, VMEM] + [VMEM] * len(aligned) + [ANY] * n_mix,
        out_specs=tuple(VMEM for _ in range(tps)),
        scratch_shapes=[
            pltpu.VMEM((mine + PAD, width), BF16),
            pltpu.VMEM((total, 8), F32),
            pltpu.SemaphoreType.DMA((n_mix,)),
        ],
        name="mix",
    )(pos, channels_of(chan_gain[None, :]), conv, *aligned, *mix_blocks)
    mix_got = [mix_terms[0]] + [shift(mix_terms[k], "tp", -k) for k in range(1, tps)]

    def added(terms, at, size):
        total = terms[0][at : at + size].astype(F32)
        for t in terms[1:]:
            total = total + t[at : at + size].astype(F32)
        return total

    sent = [shift(added(mix_got, r * n, n).astype(BF16), "rep", -r) for r in range(1, reps)]
    mix_sum = added(mix_got, 0, n)
    for t in sent:
        mix_sum = mix_sum + t.astype(F32)
    middle = (take(tokens, ci, n, 0).astype(F32) + mix_sum).astype(BF16)
    normed2 = rms_rows(middle, second_gain)

    across = [normed2] + [shift(normed2, "rep", r) for r in range(1, reps)]
    beside = [normed2] + [pair_shift(normed2, q) for q in range(1, pair)]
    local = {(0, r): [across[r]] for r in range(reps)}
    for q in range(1, pair):
        local[q, 0] = [beside[q]]
        for r in range(1, reps):
            local[q, r] = [shift(beside[q], "rep", r)]
    cells = [(q, r) for q in range(pair) for r in range(reps)]
    toks = [t for cell in cells for t in local[cell]]
    hidden = pl.pallas_call(
        functools.partial(up_kernel, all_places, len(toks), tps),
        out_shape=jax.ShapeDtypeStruct((len(cells) * n, tps * units), BF16),
        in_specs=[SMEM] + [VMEM] * tps + [ANY] * (len(toks) + tps * fss),
        out_specs=ANY,
        scratch_shapes=[
            pltpu.VMEM((len(cells) * n, width), BF16),
            pltpu.VMEM((depth, tps * units), BF16),
            pltpu.VMEM((len(cells) * n, tps * units), BF16),
            pltpu.SemaphoreType.DMA((len(toks) + tps * fss,)),
            pltpu.SemaphoreType.DMA((tps,)),
        ],
        name="up",
    )(pos, *up_scales, *toks, *up_blocks)

    per = len(cells) * n
    block_cols = width // fss
    own_pair = [
        (k, m, lambda p, m=m, k=k: (p[1] ^ m) % pair * inner + lax.rem(p[2] + inner - k, inner))
        for k in range(inner)
        for m in range(pair)
    ]
    other = [[(k, m, lambda p, m=m: (p[1] ^ m) % pair) for m in range(pair, outer)] for k in range(inner)]
    base = zi // pair * pair
    starts = [[(base * inner) * block_cols]] + [
        [((pair - base + z) * inner + (yi - k) % inner) * block_cols for z in range(pair)] for k in range(inner)
    ]
    results = []
    for part, members in enumerate([own_pair] + other):
        blocks = []
        for h in range(tps):
            cut, at = columns([down_blocks[k][h][m] for k, m, _ in members], [f for _, _, f in members])
            blocks += cut
        n_cols = len(members) * block_cols
        rep_first = part % 2 == 0
        first, second = (reps, pair) if rep_first else (pair, reps)
        size = second * n
        order = tuple(r * pair + q if rep_first else q * reps + r for q, r in cells)
        kept, sent = pl.pallas_call(
            functools.partial(down_kernel, at, tps, order, n, size),
            out_shape=(
                jax.ShapeDtypeStruct((size, n_cols), F32),
                jax.ShapeDtypeStruct((per - size, n_cols), BF16),
            ),
            in_specs=[SMEM, ANY] + [ANY] * len(blocks),
            out_specs=(VMEM, VMEM),
            scratch_shapes=[
                pltpu.VMEM((per, tps * units), BF16),
                pltpu.VMEM((tps * units, n_cols), BF16),
                pltpu.VMEM((PAD, n_cols), BF16),
                pltpu.SemaphoreType.DMA((1 + len(at) * (tps + 1),)),
            ],
        )(pos, hidden, *blocks)

        def over_rep(a, j):
            return shift(a.astype(BF16), "rep", -j)

        def over_pair(a, j):
            return pair_shift(a.astype(BF16), -j)

        send_first, send_second = (over_rep, over_pair) if rep_first else (over_pair, over_rep)
        moved = [send_first(sent[(j - 1) * size : j * size], j) for j in range(1, first)]

        def after_first(j):
            total = kept[j * n : (j + 1) * n]
            for t in moved:
                total = total + t[j * n : (j + 1) * n].astype(F32)
            return total

        ready = [after_first(j).astype(BF16) for j in range(1, second)]
        last = [send_second(a, j) for j, a in enumerate(ready, 1)]
        total = after_first(0)
        for t in last:
            total = total + t.astype(F32)
        wide = n_cols // len(starts[part])
        own_middle = [lax.dynamic_slice_in_dim(middle, start, wide, axis=1) for start in starts[part]]
        results.append((jnp.concatenate(own_middle, axis=1).astype(F32) + total).astype(BF16))

    pieces = [[shift(a, "tp", c) if c else a for a in results] for c in range(tps)]
    if block_cols % 128 == 0:
        return pl.pallas_call(
            functools.partial(final_kernel, inner, pair, block_cols, tps),
            out_shape=jax.ShapeDtypeStruct((count, width), BF16),
            in_specs=[SMEM] + [VMEM] * (len(results) * tps),
            out_specs=VMEM,
            name="final",
        )(pos, *[a for row in pieces for a in row])
    result = jnp.zeros((count, width), BF16)
    for c in range(tps):
        for part, piece in enumerate(pieces[c]):
            wide = piece.shape[1] // len(starts[part])
            for j, start in enumerate(starts[part]):
                cut = piece[:, j * wide : (j + 1) * wide]
                result = lax.dynamic_update_slice(result, cut, ((ci - c) % tps * n, start))
    return result


def solution(mesh):
    placed = (
        P(("rep", "fs"), None),
        P(),
        P("fs", "tp"),
        P("fs", "tp"),
        P("tp"),
        P("tp"),
        P(None, "tp"),
        P("tp"),
        P("tp", "fs"),
        P("fs"),
        P(),
        P("fs", "tp"),
        P("tp"),
        P("tp", "fs"),
        P("fs"),
    )

    return jax.shard_map(on_device, mesh=mesh, in_specs=placed, out_specs=P(("rep", "fs"), None), check_vma=False)
```

```python
import functools

import jax
import jax.numpy as jnp
from jax import lax
from jax.experimental import pallas as pl
from jax.experimental.pallas import tpu as pltpu
from jax.sharding import PartitionSpec as P


SEQ_LEN = 128
EPS = 1e-05
PAD = 16


ANY = pl.BlockSpec(memory_space=pl.ANY)
SMEM = pl.BlockSpec(memory_space=pltpu.SMEM)
VMEM = pl.BlockSpec(memory_space=pltpu.VMEM)
BF16 = jnp.bfloat16
F32 = jnp.float32


def rms_rows(rows, gain):
    values = rows.astype(F32)
    scaled = values * lax.rsqrt(jnp.mean(values * values, axis=-1, keepdims=True) + EPS)
    return (scaled * gain).astype(BF16)


def start_all(pairs, sems):
    copies = [pltpu.make_async_copy(s, d, sems.at[i]) for i, (s, d) in enumerate(pairs)]
    for c in copies:
        c.start()
    return copies


def lanes(ref, index, width):
    if ref.shape[1] == width:
        return slice(None)
    return pl.ds(pl.multiple_of(index * width, width), width)


def wait_all(copies):
    for c in copies:
        c.wait()


def glu_conv_kernel(places, offsets, rows, n_own, pos, vs, gs, taps, *refs):
    nb, n_parts = len(places), len(offsets)
    own = refs[0]
    parts = refs[1 : 1 + n_parts]
    blocks = refs[1 + n_parts : 1 + n_parts + nb]
    conv_out, stat_out, x, w, padded, sems = refs[1 + n_parts + nb :]
    n = parts[0].shape[0]
    pairs = [(own, x.at[pl.ds(0, n_own)])]
    for p in range(n_parts):
        pairs.append((parts[p], x.at[pl.ds(pl.multiple_of(offsets[p](pos), n), n)]))
    for b in range(nb):
        pairs.append((blocks[b], w.at[pl.ds(pl.multiple_of(places[b](pos) * rows, rows), rows)]))
    wait_all(start_all(pairs, sems))
    total, width = conv_out.shape
    chan = lanes(vs, pos[0], width)
    vs_own = vs[:, chan].astype(BF16).astype(F32)
    gs_own = gs[:, chan].astype(BF16).astype(F32)
    n_seq = total // SEQ_LEN
    k = taps.shape[0]
    lead = padded.shape[1] - SEQ_LEN
    both = jnp.dot(x[...], w[...], preferred_element_type=F32)
    glu = both[:, :width] * vs_own * jax.nn.sigmoid(both[:, width:] * gs_own)
    for s in range(n_seq):
        padded[s, :lead, :] = jnp.zeros((lead, width), F32)
        padded[s, lead:, :] = glu[s * SEQ_LEN : (s + 1) * SEQ_LEN, :]
    for s in range(n_seq):
        at = s * SEQ_LEN
        acc = jnp.zeros((SEQ_LEN, width), F32)
        for j in range(k):
            start = lead - (k - 1) + j
            acc = acc + taps[j : j + 1, chan] * padded[s, start : start + SEQ_LEN, :]
        conv_out[at : at + SEQ_LEN, :] = acc
    conv = conv_out[...]
    sums = jnp.sum(conv, axis=1, keepdims=True)
    squares = jnp.sum(conv * conv, axis=1, keepdims=True)
    lane = lax.broadcasted_iota(jnp.int32, (total, 128), 1)
    stat_out[...] = jnp.where(lane == 0, sums, squares).T[:8, :]


def mix_kernel(places, turns, reps, tps, n, channels, pos, gain, conv, *refs):
    nb, n_stats = len(places), len(turns)
    stats = refs[:n_stats]
    blocks = refs[n_stats : n_stats + nb]
    outs = refs[n_stats + nb : n_stats + nb + tps]
    w, columns, sems = refs[n_stats + nb + tps :]
    cols = blocks[0].shape[1]
    copies = start_all(
        [(blocks[b], w.at[:, pl.ds(pl.multiple_of(places[b](pos) * cols, cols), cols)]) for b in range(nb)],
        sems,
    )
    width = conv.shape[1]
    stat = stats[0][...]
    per = n * tps
    for s, turn in zip(stats[1:], turns[1:]):
        blocks_of = [(q - turn) % reps for q in range(reps)]
        stat = stat + jnp.concatenate([s[:, q * per : (q + 1) * per] for q in blocks_of], axis=1)
    columns[...] = stat.T
    own_gain = gain[:, lanes(gain, pos[0], width)]
    wait_all(copies)
    scale = w[width : width + 1, :].astype(F32)
    mixed = []
    for k in range(tps):
        for r in range(reps):
            at = pl.multiple_of(r * per + lax.rem(pos[3] + tps - k, tps) * n, n)
            column = columns[pl.ds(at, n), :]
            mean = column[:, 0:1] / channels
            var = column[:, 1:2] / channels - mean * mean
            v = (conv[pl.ds(at, n), :] - mean) * lax.rsqrt(var + EPS) * own_gain
            mixed.append((v / (1.0 + jnp.exp(-v))).astype(BF16))
    mixed = jnp.concatenate(mixed, axis=0)
    term = (jnp.dot(mixed, w[:width, :], preferred_element_type=F32) * scale).astype(BF16)
    for k in range(tps):
        outs[k][...] = term[k * reps * n : (k + 1) * reps * n, :]


def up_kernel(places, n_tok, tps, pos, *refs):
    nb = len(places)
    scales = refs[:tps]
    refs = refs[tps:]
    toks = refs[:n_tok]
    ups = refs[n_tok : n_tok + tps * nb]
    out, x, wu, stage, sems, out_sems = refs[n_tok + tps * nb :]
    units = wu.shape[1] // tps
    rows = ups[0].shape[0]
    n = toks[0].shape[0]
    pairs = [(t, x.at[pl.ds(i * n, n)]) for i, t in enumerate(toks)]
    for k in range(tps):
        for b in range(nb):
            at = pl.ds(pl.multiple_of(places[b](pos) * rows, rows), rows)
            pairs.append((ups[k * nb + b], wu.at[at, pl.ds(k * units, units)]))
    copies = start_all(pairs, sems)
    wait_all(copies[:n_tok])
    step = min(x.shape[0], 512)
    writes = []
    for k in range(tps):
        wait_all(copies[n_tok + k * nb : n_tok + (k + 1) * nb])
        for at in range(0, x.shape[0], step):
            w = wu[:, k * units : (k + 1) * units]
            up = jnp.dot(x[at : at + step, :], w, preferred_element_type=F32) * scales[k][...].astype(BF16).astype(F32)
            stage[at : at + step, k * units : (k + 1) * units] = jnp.square(jnp.maximum(up, 0.0)).astype(BF16)
        cut = pl.ds(k * units, units)
        writes.append(pltpu.make_async_copy(stage.at[:, cut], out.at[:, cut], out_sems.at[k]))
        writes[-1].start()
    wait_all(writes)


def down_kernel(places, tps, order, n, kept_rows, pos, hidden, *refs):
    nd = len(places)
    downs = refs[: tps * nd]
    kept, sent, h, wd, ws, sems = refs[tps * nd :]
    cols = downs[0].shape[1]
    units = h.shape[1] // tps
    pairs = [(hidden, h)]
    for b in range(nd):
        at = pl.ds(pl.multiple_of(places[b](pos) * cols, cols), cols)
        for k in range(tps):
            pairs.append((downs[k * nd + b].at[pl.ds(0, units)], wd.at[pl.ds(k * units, units), at]))
        pairs.append((downs[b].at[pl.ds(units, PAD)], ws.at[:, at]))
    wait_all(start_all(pairs, sems))
    scale = ws[0:1, :].astype(F32)
    term = jnp.dot(h[...], wd[...], preferred_element_type=F32) * scale
    for j, to in enumerate(order):
        rows = term[j * n : (j + 1) * n, :]
        if to * n < kept_rows:
            kept[to * n : (to + 1) * n, :] = rows
        else:
            sent[to * n - kept_rows : (to + 1) * n - kept_rows, :] = rows.astype(BF16)


def final_kernel(inner, pair, cols, tps, pos, *refs):
    out, sems = refs[-2:]
    n_parts = 1 + inner
    pairs = []
    base = pos[1] - lax.rem(pos[1], pair)
    for c in range(tps):
        parts = refs[c * n_parts : (c + 1) * n_parts]
        n = parts[0].shape[0]
        rows = pl.ds(pl.multiple_of(lax.rem(pos[3] + tps - c, tps) * n, n), n)
        wide = parts[0].shape[1]
        pairs.append((parts[0], out.at[rows, pl.ds(pl.multiple_of(base * inner * cols, cols), wide)]))
        for k in range(inner):
            for z in range(pair):
                block = (pair - base + z) * inner + lax.rem(pos[2] + inner - k, inner)
                at = pl.multiple_of(block * cols, cols)
                pairs.append((parts[1 + k].at[:, pl.ds(z * cols, cols)], out.at[rows, pl.ds(at, cols)]))
    wait_all(start_all(pairs, sems))


def shift(array, axis, by):
    size = lax.axis_size(axis)
    return lax.ppermute(array, axis, [(i, (i + by) % size) for i in range(size)])


def on_device(
    tokens,
    first_gain,
    value_weight,
    gate_weight,
    value_scale,
    gate_scale,
    conv_taps,
    chan_gain,
    mixout_weight,
    mixout_scale,
    second_gain,
    up_weight,
    up_scale,
    down_weight,
    down_scale,
):
    reps, fss, tps = lax.axis_size("rep"), lax.axis_size("fs"), lax.axis_size("tp")
    outer, pair = 4, 2
    inner = fss // outer
    xi, fi, ci = lax.axis_index("rep"), lax.axis_index("fs"), lax.axis_index("tp")
    zi, yi = fi // inner, fi % inner
    count, width = tokens.shape
    n = count // tps

    def along(a, to):
        return lax.ppermute(a, "fs", [(o * inner + i, to(o, i)) for o in range(outer) for i in range(inner)])

    def z_swap(a, m):
        return along(a, lambda o, i: (o ^ m) * inner + i)

    def y_shift(a, s):
        return along(a, lambda o, i: o * inner + (i + s) % inner)

    def pair_shift(a, s):
        return along(a, lambda o, i: (o // pair * pair + (o + s) % pair) * inner + i)

    pos = jnp.stack([xi, zi, yi, ci]).astype(jnp.int32)

    def spread(got):
        if inner <= 2:
            return [list(got.values())] + [[y_shift(b, k) for b in got.values()] for k in range(1, inner)]
        stack = jnp.stack(list(got.values()))
        moved = [y_shift(stack, k) for k in range(1, inner)]
        return [list(got.values())] + [[m[s] for s in range(outer)] for m in moved]

    def gather(block):
        got = {"0": block, "a": z_swap(block, 1), "b": z_swap(block, 2)}
        got["c"] = z_swap(got["b"], 1)
        return spread(got)

    def exchange(blocks):
        got = {"0": blocks[0]}
        for m in range(1, outer):
            got[str(m)] = z_swap(blocks[m % pair], m)
        return spread(got)

    def place(m, k):
        return lambda p: (p[1] ^ m) * inner + lax.rem(p[2] + inner - k, inner)

    all_places = [place(m, k) for k in range(inner) for m in range(outer)]

    def flat(blocks):
        return [b for row in blocks for b in row]

    def take(a, at, size, axis):
        return lax.dynamic_slice_in_dim(a, at * size, size, axis=axis)

    mine = value_weight.shape[1] // reps
    vg = jnp.concatenate(
        [take(value_weight, xi, mine, 1).astype(BF16), take(gate_weight, xi, mine, 1).astype(BF16)], axis=1
    )

    def channels_of(a):
        return a if mine % 128 == 0 else take(a, xi, mine, 1)

    vg_blocks = flat(gather(vg))

    def with_scale(block, scale):
        rows = jnp.broadcast_to(scale.astype(BF16)[None, :], (PAD, scale.shape[0]))
        return jnp.concatenate([block.astype(BF16), rows], axis=0)

    def columns(blocks, at):
        cols = blocks[0].shape[1]
        if cols % 128 == 0:
            return blocks, at
        joined = jnp.zeros((blocks[0].shape[0], cols * len(blocks)), BF16)
        for block, spot in zip(blocks, at):
            joined = lax.dynamic_update_slice_in_dim(joined, block, spot(pos) * cols, axis=1)
        return [joined], [lambda p: 0]

    mix_own = with_scale(take(mixout_weight, xi, mine, 0), mixout_scale)
    mix_blocks, mix_places = columns(flat(gather(mix_own)), all_places)

    normed = rms_rows(tokens, first_gain)
    half = take(normed, ci, n, 0)
    parts, offsets = [], []
    for r in range(1, reps):
        moved = shift(half, "rep", r)
        for k in range(tps):
            parts.append(shift(moved, "tp", k) if k else moved)
            offsets.append(lambda p, r=r, k=k: r * count + lax.rem(p[3] + tps - k, tps) * n)

    groups = reps * pair
    units = up_weight.shape[1] // groups

    at_pair = [xi * pair + (zi + s) % pair for s in range(pair)]
    ups = [take(up_weight, g, units, 1).astype(BF16) for g in at_pair]
    downs = [with_scale(take(down_weight, g, units, 0), down_scale) for g in at_pair]

    def share(parts):
        if tps == 2:
            return [[blocks, [shift(b, "tp", 1) for b in blocks]] for blocks in parts]
        shared = []
        for blocks in parts:
            stack = jnp.stack(blocks)
            moved = [shift(stack, "tp", k) for k in range(1, tps)]
            shared.append([blocks] + [[m[s] for s in range(len(blocks))] for m in moved])
        return shared

    up_blocks = exchange(ups)
    up_blocks = share(up_blocks)
    up_blocks = [b for k in range(tps) for part in up_blocks for b in part[k]]
    down_blocks = exchange(downs)
    down_blocks = share(down_blocks)
    own_scale = take(up_scale, at_pair[0], units, 0)[None, :]
    up_scales = [own_scale] + [shift(own_scale, "tp", k) for k in range(1, tps)]

    total = reps * count
    rows = value_weight.shape[0]
    depth = rows * fss
    lead = -(-(conv_taps.shape[0] - 1) // 8) * 8
    conv, stat = pl.pallas_call(
        functools.partial(glu_conv_kernel, all_places, offsets, rows, count),
        out_shape=(
            jax.ShapeDtypeStruct((total, mine), F32),
            jax.ShapeDtypeStruct((8, total), F32),
        ),
        in_specs=[SMEM, VMEM, VMEM, VMEM] + [ANY] * (1 + len(parts) + fss),
        out_specs=(VMEM, VMEM),
        scratch_shapes=[
            pltpu.VMEM((total, width), BF16),
            pltpu.VMEM((depth, 2 * mine), BF16),
            pltpu.VMEM((total // SEQ_LEN, SEQ_LEN + lead, mine), F32),
            pltpu.SemaphoreType.DMA((1 + len(parts) + fss,)),
        ],
        name="glu_conv",
    )(pos, channels_of(value_scale[None, :]), channels_of(gate_scale[None, :]), channels_of(conv_taps), normed, *parts, *vg_blocks)

    stats = [stat]
    for r in range(reps):
        for k in range(tps):
            if r or k:
                to = [
                    (i * tps + j, (i + r) % reps * tps + (j + k) % tps)
                    for i in range(reps)
                    for j in range(tps)
                ]
                stats.append((r, lax.ppermute(stat, ("rep", "tp"), to)))
    turns = [0] + [r for r, _ in stats[1:]]
    aligned = [stat] + [t for _, t in stats[1:]]
    n_mix = len(mix_blocks)
    mix_terms = pl.pallas_call(
        functools.partial(mix_kernel, mix_places, turns, reps, tps, n, float(mine * reps * tps)),
        out_shape=tuple(jax.ShapeDtypeStruct((reps * n, width), BF16) for _ in range(tps)),
        in_specs=[SMEM, VMEM, VMEM] + [VMEM] * len(aligned) + [ANY] * n_mix,
        out_specs=tuple(VMEM for _ in range(tps)),
        scratch_shapes=[
            pltpu.VMEM((mine + PAD, width), BF16),
            pltpu.VMEM((total, 8), F32),
            pltpu.SemaphoreType.DMA((n_mix,)),
        ],
        name="mix",
    )(pos, channels_of(chan_gain[None, :]), conv, *aligned, *mix_blocks)
    mix_got = [mix_terms[0]] + [shift(mix_terms[k], "tp", -k) for k in range(1, tps)]

    def added(terms, at, size):
        total = terms[0][at : at + size].astype(F32)
        for t in terms[1:]:
            total = total + t[at : at + size].astype(F32)
        return total

    sent = [shift(added(mix_got, r * n, n).astype(BF16), "rep", -r) for r in range(1, reps)]
    mix_sum = added(mix_got, 0, n)
    for t in sent:
        mix_sum = mix_sum + t.astype(F32)
    middle = (take(tokens, ci, n, 0).astype(F32) + mix_sum).astype(BF16)
    normed2 = rms_rows(middle, second_gain)

    across = [normed2] + [shift(normed2, "rep", r) for r in range(1, reps)]
    beside = [normed2] + [pair_shift(normed2, q) for q in range(1, pair)]
    local = {(0, r): [across[r]] for r in range(reps)}
    for q in range(1, pair):
        local[q, 0] = [beside[q]]
        for r in range(1, reps):
            local[q, r] = [shift(beside[q], "rep", r)]
    cells = [(q, r) for q in range(pair) for r in range(reps)]
    toks = [t for cell in cells for t in local[cell]]
    hidden = pl.pallas_call(
        functools.partial(up_kernel, all_places, len(toks), tps),
        out_shape=jax.ShapeDtypeStruct((len(cells) * n, tps * units), BF16),
        in_specs=[SMEM] + [VMEM] * tps + [ANY] * (len(toks) + tps * fss),
        out_specs=ANY,
        scratch_shapes=[
            pltpu.VMEM((len(cells) * n, width), BF16),
            pltpu.VMEM((depth, tps * units), BF16),
            pltpu.VMEM((len(cells) * n, tps * units), BF16),
            pltpu.SemaphoreType.DMA((len(toks) + tps * fss,)),
            pltpu.SemaphoreType.DMA((tps,)),
        ],
        name="up",
    )(pos, *up_scales, *toks, *up_blocks)

    per = len(cells) * n
    block_cols = width // fss
    own_pair = [
        (k, m, lambda p, m=m, k=k: (p[1] ^ m) % pair * inner + lax.rem(p[2] + inner - k, inner))
        for k in range(inner)
        for m in range(pair)
    ]
    other = [[(k, m, lambda p, m=m: (p[1] ^ m) % pair) for m in range(pair, outer)] for k in range(inner)]
    base = zi // pair * pair
    starts = [[(base * inner) * block_cols]] + [
        [((pair - base + z) * inner + (yi - k) % inner) * block_cols for z in range(pair)] for k in range(inner)
    ]
    results = []
    for part, members in enumerate([own_pair] + other):
        blocks = []
        for h in range(tps):
            cut, at = columns([down_blocks[k][h][m] for k, m, _ in members], [f for _, _, f in members])
            blocks += cut
        n_cols = len(members) * block_cols
        rep_first = part % 2 == 0
        first, second = (reps, pair) if rep_first else (pair, reps)
        size = second * n
        order = tuple(r * pair + q if rep_first else q * reps + r for q, r in cells)
        kept, sent = pl.pallas_call(
            functools.partial(down_kernel, at, tps, order, n, size),
            out_shape=(
                jax.ShapeDtypeStruct((size, n_cols), F32),
                jax.ShapeDtypeStruct((per - size, n_cols), BF16),
            ),
            in_specs=[SMEM, ANY] + [ANY] * len(blocks),
            out_specs=(VMEM, VMEM),
            scratch_shapes=[
                pltpu.VMEM((per, tps * units), BF16),
                pltpu.VMEM((tps * units, n_cols), BF16),
                pltpu.VMEM((PAD, n_cols), BF16),
                pltpu.SemaphoreType.DMA((1 + len(at) * (tps + 1),)),
            ],
        )(pos, hidden, *blocks)

        def over_rep(a, j):
            return shift(a.astype(BF16), "rep", -j)

        def over_pair(a, j):
            return pair_shift(a.astype(BF16), -j)

        send_first, send_second = (over_rep, over_pair) if rep_first else (over_pair, over_rep)
        moved = [send_first(sent[(j - 1) * size : j * size], j) for j in range(1, first)]

        def after_first(j):
            total = kept[j * n : (j + 1) * n]
            for t in moved:
                total = total + t[j * n : (j + 1) * n].astype(F32)
            return total

        ready = [after_first(j).astype(BF16) for j in range(1, second)]
        last = [send_second(a, j) for j, a in enumerate(ready, 1)]
        total = after_first(0)
        for t in last:
            total = total + t.astype(F32)
        wide = n_cols // len(starts[part])
        own_middle = [lax.dynamic_slice_in_dim(middle, start, wide, axis=1) for start in starts[part]]
        results.append((jnp.concatenate(own_middle, axis=1).astype(F32) + total).astype(BF16))

    pieces = [[shift(a, "tp", c) if c else a for a in results] for c in range(tps)]
    if block_cols % 128 == 0:
        return pl.pallas_call(
            functools.partial(final_kernel, inner, pair, block_cols, tps),
            out_shape=jax.ShapeDtypeStruct((count, width), BF16),
            in_specs=[SMEM] + [ANY] * (len(results) * tps),
            out_specs=ANY,
            scratch_shapes=[pltpu.SemaphoreType.DMA((tps * (1 + inner * pair),))],
            name="final",
        )(pos, *[a for row in pieces for a in row])
    result = jnp.zeros((count, width), BF16)
    for c in range(tps):
        for part, piece in enumerate(pieces[c]):
            wide = piece.shape[1] // len(starts[part])
            for j, start in enumerate(starts[part]):
                cut = piece[:, j * wide : (j + 1) * wide]
                result = lax.dynamic_update_slice(result, cut, ((ci - c) % tps * n, start))
    return result


def solution(mesh):
    placed = (
        P(("rep", "fs"), None),
        P(),
        P("fs", "tp"),
        P("fs", "tp"),
        P("tp"),
        P("tp"),
        P(None, "tp"),
        P("tp"),
        P("tp", "fs"),
        P("fs"),
        P(),
        P("fs", "tp"),
        P("tp"),
        P("tp", "fs"),
        P("fs"),
    )

    return jax.shard_map(on_device, mesh=mesh, in_specs=placed, out_specs=P(("rep", "fs"), None), check_vma=False)
```
